32 devices in a mesh: ep: 8 (over z, x), tp: 4 (over y, core).
Axes of the slice: x: 2, y: 2, z: 4, core: 2. Of those that a mesh axis runs over, the one named last changes fastest.
Arguments:
- tokens: bfloat16 [192, 4096], P('ep'), may hold values from -6 to 6
- delta_state: float32 [192, 16, 128, 128], P('ep', 'tp'), may hold values from -0.625 to 0.625
- attn_gain: float32 [4096], replicated, may hold values from 0.1 to 1.9
- query_weight: bfloat16 [4096, 2048], P('ep', 'tp'), may hold values from -0.09375 to 0.09375
- key_weight: bfloat16 [4096, 2048], P('ep', 'tp'), may hold values from -0.09375 to 0.09375
- value_weight: bfloat16 [4096, 2048], P('ep', 'tp'), may hold values from -0.09375 to 0.09375
- decay_weight: bfloat16 [4096, 16], replicated, may hold values from -0.09375 to 0.09375
- beta_weight: bfloat16 [4096, 16], replicated, may hold values from -0.09375 to 0.09375
- decay_rate: float32 [16], P('tp'), may hold values from 0.05 to 3
- head_gain: float32 [128], replicated, may hold values from 0.1 to 1.9
- output_weight: bfloat16 [2048, 4096], P('tp'), may hold values from -0.125 to 0.125
- ffn_gain: float32 [4096], replicated, may hold values from 0.1 to 1.9
- expert_ids: int32 [192, 2], P('ep'), may hold values from 0 to 7, all different within a row; in each aligned block of 24 rows (0 to 23, 24 to 47, ...) at most 12 rows name the same one
- group_prob: float32 [192], P('ep'), may hold values from 0.3 to 1
- expert_logit: float32 [192, 2], P('ep'), may hold values from -8 to 8
- expert_gate: bfloat16 [8, 4096, 1024], P('ep', None, 'tp'), may hold values from -0.09375 to 0.09375
- expert_up: bfloat16 [8, 4096, 1024], P('ep', None, 'tp'), may hold values from -0.09375 to 0.09375
- expert_down: bfloat16 [8, 1024, 4096], P('ep', 'tp'), may hold values from -0.1875 to 0.1875
- dense_gate: bfloat16 [4096, 4096], P('tp', 'ep'), may hold values from -0.09375 to 0.09375
- dense_up: bfloat16 [4096, 4096], P('tp', 'ep'), may hold values from -0.09375 to 0.09375
- dense_down: bfloat16 [4096, 4096], P('ep', 'tp'), may hold values from -0.09375 to 0.09375
- dense_mix: float32 [4096], P('tp'), may hold values from -3 to 3
Outputs:
- mixed_out: bfloat16 [192, 4096], P('ep', 'tp')
- new_state: float32 [192, 16, 128, 128], P('ep', 'tp')
The draws below stay inside these ranges and needn't reach their ends.
Inputs may be any that keep to these rules, and one draw needn't show every extreme that they name: `expert_ids`: each row names 2 different experts. Among the rows of one device (aligned blocks of 24 rows) no expert is named by more than 12 rows, and in every draw some expert reaches 12 in some block.
All inputs are finite; a program needn't handle non-finite values.
Results may differ from the reference program's by a relative error of at most 0.02.
Values may be sent and summed in bfloat16 or wider, within the bound.
A program may use at most 64 MiB of HBM per device.

```python
import math
import jax
import jax.numpy as jnp
import numpy as np
from jax import lax

D = 4096
HEADS = 16
HEAD = 128
FE = 1024
FD = 4096
TOPK = 2
SEQ_DEV = 24
BATCH = 192
EXPERTS = 8
CAP = 12
N_EP = 8
N_TP = 4


def block_scale(stream_key, extent, pieces, low, top_value):
    factor_of = 1.0
    for dim, blocks in pieces:
        heights = jax.random.uniform(jax.random.fold_in(jax.random.fold_in(stream_key, 6), dim), (blocks,), jnp.float32, low / len(pieces), top_value / len(pieces))
        factor_of = factor_of * jnp.repeat(jnp.exp(heights), extent[dim] // blocks).reshape((-1,) + (1,) * (len(extent) - 1 - dim))
    return factor_of


def routed_block(own_key, own, number, rows, count, top, reach, slope):
    sequence = jax.random.permutation(own_key, count)
    crowded, usual = portions_of(count, rows * top, reach, slope, True), portions_of(count, rows * top, reach, slope, False)
    places = jnp.arange(count)

    def named(lengths, offset_by):
        used = int((lengths > 0).sum())
        fixed = max(1, used // 4)
        shifted = fixed + (places - fixed + offset_by * (used - fixed)) % max(1, count - fixed)
        return jnp.zeros((count,), jnp.int32).at[sequence[jnp.where(places < fixed, places, shifted)]].set(jnp.asarray(lengths, jnp.int32))

    lengths = jnp.where(number % 4 == 0, named(crowded, number // 4), named(usual, number - number // 4 - 1))
    mixed = jax.random.permutation(jax.random.fold_in(own, 3), count)
    giver, receiver = mixed[0:count // 2 * 2:2], mixed[1:count // 2 * 2:2]
    slack = jnp.minimum(lengths[giver] - 1, reach - lengths[receiver]) // 2
    slack = jnp.where((giver == sequence[0]) | (receiver == sequence[0]) | (lengths[receiver] == 0), 0, jnp.maximum(slack, 0))
    shifted = jax.random.randint(jax.random.fold_in(own, 4), (count // 2,), 0, 1 << 20) % (slack + 1)
    lengths = lengths.at[giver].add(-shifted).at[receiver].add(shifted)
    items = jnp.searchsorted(jnp.cumsum(lengths), jnp.arange(rows * top), side="right").astype(jnp.int32)
    table = items.reshape(top, rows).T
    table = table[jax.random.permutation(jax.random.fold_in(own, 1), rows)]
    offset_by = jax.random.randint(jax.random.fold_in(own, 2), (rows, 1), 0, top)
    return jnp.take_along_axis(table, (jnp.arange(top)[None, :] + offset_by) % top, axis=1)


def portions_of(count, total, most, lean, full):
    portions = [(1 << 20) // math.isqrt(grade ** lean) + 1 for grade in range(1, count + 1)]
    largest = most if full else min(most, max(-(-total // count), total * portions[0] // sum(portions)))
    least = 1 if total - largest >= count - 1 else 0
    holding, rest = [largest] + [least] * (count - 1), total - largest - least * (count - 1)
    while rest > 0:
        free = [i for i in range(1, count) if holding[i] < largest] or [i for i in range(1, count) if holding[i] < most]
        whole, budget = sum([portions[i] for i in free]), rest
        for i in free:
            more = min(most - holding[i], max(1, budget * portions[i] // whole), rest)
            holding[i] = holding[i] + more
            rest = rest - more
    return np.array(holding)


def bell_draw(stream_key, extent, width, most, pieces=(), held_as=jnp.bfloat16):
    drawn = width * jax.random.normal(stream_key, extent, jnp.float32)
    if pieces:
        drawn = drawn * block_scale(stream_key, extent, pieces, -0.22, 0.18)
    return jnp.clip(drawn, -most, most).astype(held_as)


def setup_inputs(seed: int = 0) -> dict:
    keys = jax.random.split(jax.random.key(seed), 23)
    tokens = bell_draw(keys[0], (BATCH, D), 1.0, 6.0, ((0, 8),))
    delta_state = bell_draw(keys[1], (BATCH, HEADS, HEAD, HEAD), 0.1, 0.625, ((0, 8), (1, 4)), jnp.float32)
    attn_gain = jnp.clip(1.0 + 0.18 * jax.random.normal(keys[2], (D,), jnp.float32), 0.1, 1.9)
    query_weight = bell_draw(keys[3], (D, HEADS * HEAD), D ** -0.5, 0.09375, ((0, 8), (1, 4)))
    key_weight = bell_draw(keys[4], (D, HEADS * HEAD), D ** -0.5, 0.09375, ((0, 8), (1, 4)))
    value_weight = bell_draw(keys[5], (D, HEADS * HEAD), D ** -0.5, 0.09375, ((0, 8), (1, 4)))
    decay_weight = bell_draw(keys[6], (D, HEADS), D ** -0.5, 0.09375)
    beta_weight = bell_draw(keys[7], (D, HEADS), D ** -0.5, 0.09375)
    decay_rate = jnp.clip(jnp.exp(math.log(3.0) - 4.0943445 * jax.random.uniform(keys[8], (HEADS,), jnp.float32) ** block_scale(keys[8], (HEADS,), ((0, 4),), -0.2, 0.2)), 0.05, 3.0)
    head_gain = jnp.clip(1.0 + 0.18 * jax.random.normal(keys[9], (HEAD,), jnp.float32), 0.1, 1.9)
    output_weight = bell_draw(keys[10], (HEADS * HEAD, D), (HEADS * HEAD) ** -0.5, 0.125, ((0, 4),))
    ffn_gain = jnp.clip(1.0 + 0.18 * jax.random.normal(keys[11], (D,), jnp.float32), 0.1, 1.9)
    expert_ids_keys = jax.random.split(jax.random.fold_in(keys[12], 1), BATCH // SEQ_DEV)
    expert_ids_turns = jax.random.permutation(jax.random.fold_in(keys[12], 3), BATCH // SEQ_DEV)
    expert_ids = jax.vmap(lambda own, number: routed_block(jax.random.fold_in(keys[12], 2), own, number, SEQ_DEV, EXPERTS, TOPK, CAP, 2))(expert_ids_keys, expert_ids_turns).reshape((BATCH, TOPK))
    group_prob = jnp.clip(0.3 + 0.7 * jax.random.uniform(keys[13], (BATCH,), jnp.float32) ** block_scale(keys[13], (BATCH,), ((0, 8),), -0.2, 0.2), 0.3, 1.0)
    expert_logit = bell_draw(keys[14], (BATCH, TOPK), 1.5, 8.0, ((0, 8),), jnp.float32)
    expert_gate = bell_draw(keys[15], (EXPERTS, D, FE), D ** -0.5, 0.09375, ((0, 8), (2, 4)))
    expert_up = bell_draw(keys[16], (EXPERTS, D, FE), D ** -0.5, 0.09375, ((0, 8), (2, 4)))
    expert_down = bell_draw(keys[17], (EXPERTS, FE, D), FE ** -0.5, 0.1875, ((0, 8), (1, 4)))
    dense_gate = bell_draw(keys[18], (D, FD), D ** -0.5, 0.09375, ((0, 4), (1, 8)))
    dense_up = bell_draw(keys[19], (D, FD), D ** -0.5, 0.09375, ((0, 4), (1, 8)))
    dense_down = bell_draw(keys[20], (FD, D), FD ** -0.5, 0.09375, ((0, 8), (1, 4)))
    dense_mix = jnp.clip(jax.random.uniform(keys[21], (D,), jnp.float32, -3.0, 3.0) * block_scale(keys[21], (D,), ((0, 4),), -0.4, 0.0), -3.0, 3.0)
    return {"tokens": tokens, "delta_state": delta_state, "attn_gain": attn_gain, "query_weight": query_weight, "key_weight": key_weight, "value_weight": value_weight, "decay_weight": decay_weight, "beta_weight": beta_weight, "decay_rate": decay_rate, "head_gain": head_gain, "output_weight": output_weight, "ffn_gain": ffn_gain, "expert_ids": expert_ids, "group_prob": group_prob, "expert_logit": expert_logit, "expert_gate": expert_gate, "expert_up": expert_up, "expert_down": expert_down, "dense_gate": dense_gate, "dense_up": dense_up, "dense_down": dense_down, "dense_mix": dense_mix}


EPS = 1e-06

def rms_scale(values, gain):
    mean_sq = lax.optimization_barrier(jnp.mean(values * values, axis=-1, keepdims=True))
    return values * lax.rsqrt(mean_sq + EPS) * gain

def unit_rows(values):
    return values * lax.rsqrt(lax.optimization_barrier(jnp.sum(values * values, axis=-1, keepdims=True)) + EPS)

def rounded_back(values):
    return lax.optimization_barrier(values.astype(jnp.bfloat16)).astype(jnp.float32)

def block_sum(left, right, blocks):
    size = left.shape[1] // blocks
    total = jnp.zeros((left.shape[0], right.shape[1]), jnp.float32)
    for index in range(blocks):
        part = jnp.dot(left[:, index * size:(index + 1) * size], right[index * size:(index + 1) * size], preferred_element_type=jnp.float32)
        total = total + rounded_back(part)
    return total

def reference(tokens, delta_state, attn_gain, query_weight, key_weight, value_weight, decay_weight, beta_weight, decay_rate, head_gain, output_weight, ffn_gain, expert_ids, group_prob, expert_logit, expert_gate, expert_up, expert_down, dense_gate, dense_up, dense_down, dense_mix):
    residual = tokens.astype(jnp.float32)
    normed = rms_scale(residual, attn_gain).astype(jnp.bfloat16)

    def heads_of(weight):
        product = jnp.dot(normed, weight, preferred_element_type=jnp.float32)
        return rounded_back(product).reshape(BATCH, HEADS, HEAD)
    query_unit = unit_rows(heads_of(query_weight)) * HEAD ** (-0.5)
    key_unit = unit_rows(heads_of(key_weight))
    value_heads = heads_of(value_weight)
    decay = jnp.exp(-decay_rate * jax.nn.softplus(jnp.dot(normed, decay_weight, preferred_element_type=jnp.float32)))
    beta_gate = jax.nn.sigmoid(jnp.dot(normed, beta_weight, preferred_element_type=jnp.float32))
    recalled = jnp.einsum('bhk,bhkv->bhv', key_unit, delta_state, precision=lax.Precision.HIGHEST)
    correction = beta_gate[..., None] * (value_heads - decay[..., None] * recalled)
    new_state = decay[..., None, None] * delta_state + key_unit[..., :, None] * correction[..., None, :]
    read_out = jnp.einsum('bhk,bhkv->bhv', query_unit, new_state, precision=lax.Precision.HIGHEST)
    head_out = rms_scale(read_out, head_gain).astype(jnp.bfloat16).reshape(BATCH, HEADS * HEAD)
    attn_sum = block_sum(head_out, output_weight, N_TP)
    middle = residual + attn_sum
    ffn_in = rms_scale(middle, ffn_gain).astype(jnp.bfloat16)
    dense_pre_gate = block_sum(ffn_in, dense_gate, N_TP)
    dense_pre_up = block_sum(ffn_in, dense_up, N_TP)
    dense_hidden = (jax.nn.silu(dense_pre_gate) * dense_pre_up).astype(jnp.bfloat16)
    dense_out = jnp.dot(dense_hidden, dense_down, preferred_element_type=jnp.float32)
    pairs = SEQ_DEV * TOPK
    block_ids = expert_ids.reshape(N_EP, pairs)
    onehot = (block_ids[:, :, None] == jnp.arange(EXPERTS, dtype=jnp.int32)[None, None, :]).astype(jnp.int32)
    ranks = lax.optimization_barrier(jnp.sum(onehot * (jnp.cumsum(onehot, axis=1) - 1), axis=2))
    sources = jnp.arange(N_EP, dtype=jnp.int32)[:, None]
    places = (block_ids * (N_EP * CAP) + sources * CAP + ranks).reshape(-1).astype(jnp.int32)
    repeated = jnp.repeat(ffn_in, TOPK, axis=0)
    slots = jnp.zeros((EXPERTS * N_EP * CAP, D), jnp.bfloat16).at[places].set(repeated)
    slots = slots.reshape(EXPERTS, N_EP * CAP, D)

    def one_expert(inputs):
        arrived, gate_w, up_w, down_w = inputs
        gate_vals = jnp.dot(arrived, gate_w, preferred_element_type=jnp.float32)
        up_vals = jnp.dot(arrived, up_w, preferred_element_type=jnp.float32)
        expert_hidden = (jax.nn.silu(gate_vals) * up_vals).astype(jnp.bfloat16)
        return block_sum(expert_hidden, down_w, N_TP).astype(jnp.bfloat16)
    expert_result = lax.map(one_expert, (slots, expert_gate, expert_up, expert_down))
    picked = jnp.take(expert_result.reshape(EXPERTS * N_EP * CAP, D), places, axis=0)
    picked = picked.astype(jnp.float32).reshape(BATCH, TOPK, D)
    logit_exp = jnp.exp(expert_logit)
    route_weight = group_prob[:, None] * logit_exp / lax.optimization_barrier(jnp.sum(logit_exp, axis=1, keepdims=True))
    expert_mix = lax.optimization_barrier(jnp.sum(route_weight[..., None] * picked, axis=1))
    mixed_out = (middle + jax.nn.sigmoid(dense_mix) * dense_out + expert_mix).astype(jnp.bfloat16)
    return (mixed_out, new_state)
```

```python
import functools

import jax
import jax.numpy as jnp
from jax import lax
from jax.experimental import pallas as pl
from jax.experimental.pallas import tpu as pltpu
from jax.sharding import PartitionSpec as P

EPS = 1e-06
BF = jnp.bfloat16
F32 = jnp.float32
MESH = pl.DeviceIdType.MESH


def dot(left, right):
    return jnp.dot(left, right, preferred_element_type=F32)


def silu(values):
    return values / (1.0 + jnp.exp(-values))


def kernel(dims, *refs):
    n_ep, n_tp, rows, width, heads, slots, topk, n_in, n_weights = dims
    inputs, refs = refs[:n_in], refs[n_in:]
    (tokens, attn_gain, decay_rate, head_gain, ffn_gain, ids, group_prob, logit, mix) = inputs[:9]
    hbm = inputs[9:]
    out, key_out, corr_out, decay_out = refs[:4]
    held = refs[4 : 4 + n_weights]
    refs = refs[4 + n_weights :]
    state, w_decay, w_beta, w_q, w_k, w_v, w_o, w_dg, w_du, w_eg, w_eu, w_ed, w_dd = held
    (
        n_send, n_recv, q_send, q_recv, c_send, c_recv, kq, recall, head_out,
        a_send, a_recv, s_recv, middle_ref, x_all, g_all, d_send, d_recv, h_all,
        e_send, e_recv, f_send, f_recv, load_sem, ep_send, ep_recv, tp_send, tp_recv,
    ) = refs
    me = lax.axis_index("ep")
    my = lax.axis_index("tp")
    chunk = width // n_tp
    depth = width // n_ep
    batch = n_ep * rows
    local = heads * 128

    loads = [
        pltpu.make_async_copy(src, dst, load_sem.at[i])
        for i, (src, dst) in enumerate(zip(hbm, held))
    ]
    state_i, decay_i, beta_i, q_i, k_i, v_i, o_i, dg_i, du_i, eg_i, eu_i, ed_i, dd_i = range(13)
    order = (decay_i, beta_i, q_i, k_i, v_i, state_i, o_i, dg_i, du_i, eg_i, eu_i, ed_i, dd_i)

    ep_peers = [lax.rem(me + d, n_ep) for d in range(1, n_ep)]
    tp_peers = [lax.rem(my + d, n_tp) for d in range(1, n_tp)]
    barrier = pltpu.get_barrier_semaphore()
    for p in ep_peers:
        pl.semaphore_signal(barrier, inc=1, device_id=(p, my), device_id_type=MESH)
    for p in tp_peers:
        pl.semaphore_signal(barrier, inc=1, device_id=(me, p), device_id_type=MESH)
    for i in order:
        loads[i].start()

    def ep_copy(phase, src, dst, peer, source):
        return pltpu.make_async_remote_copy(
            src_ref=src, dst_ref=dst,
            send_sem=ep_send.at[phase, peer], recv_sem=ep_recv.at[phase, source],
            device_id=(peer, my), device_id_type=MESH,
        )

    def tp_copy(phase, src, dst, peer, source):
        return pltpu.make_async_remote_copy(
            src_ref=src, dst_ref=dst,
            send_sem=tp_send.at[phase, peer], recv_sem=tp_recv.at[phase, source],
            device_id=(me, peer), device_id_type=MESH,
        )

    def exchange(copy, phase, peers, mine, src_of, dst):
        for p in peers:
            copy(phase, src_of(p), dst.at[mine], p, mine).start()

        def arrived():
            for p in peers:
                done = copy(phase, src_of(p), dst.at[p], p, p)
                done.wait_recv()
                done.wait_send()

        return arrived

    x = tokens[...].astype(F32)
    mean_sq = jnp.mean(x * x, axis=-1, keepdims=True)
    normed = (x * lax.rsqrt(mean_sq + EPS) * attn_gain[...]).astype(BF)
    for p in range(n_ep):
        n_send[p] = normed[:, p * depth : (p + 1) * depth]
    pl.semaphore_wait(barrier, n_ep + n_tp - 2)
    wait_n = exchange(ep_copy, 0, ep_peers, me, lambda p: n_send.at[p], n_recv)
    n_recv[me] = n_send[me]

    logit_exp = jnp.exp(logit[...])
    route = group_prob[...] * logit_exp / jnp.sum(logit_exp, axis=1, keepdims=True)
    names = ids[...]
    for p in range(n_ep):
        coef = jnp.sum(jnp.where(names == p, route, 0.0), axis=1, keepdims=True)
        c_send[p] = jnp.broadcast_to(coef, (rows, 128))
    loads[decay_i].wait()
    loads[beta_i].wait()
    decay_pre = dot(normed, w_decay[...])
    beta_pre = dot(normed, w_beta[...])
    lane = lax.broadcasted_iota(jnp.int32, decay_pre.shape, 1)
    decays, betas = [], []
    for h in range(heads):
        mine = lane == my * heads + h
        d = jnp.sum(jnp.where(mine, decay_pre, 0.0), axis=1, keepdims=True)
        b = jnp.sum(jnp.where(mine, beta_pre, 0.0), axis=1, keepdims=True)
        soft = jnp.maximum(d, 0.0) + jnp.log1p(jnp.exp(-jnp.abs(d)))
        decays.append(jnp.exp(-decay_rate[:, h : h + 1] * soft))
        betas.append(1.0 / (1.0 + jnp.exp(-b)))
    for i in (q_i, k_i, v_i):
        loads[i].wait()

    wait_n()
    spread = n_recv[...].astype(F32).reshape(batch, depth).astype(BF)
    for j, w in enumerate((w_q, w_k, w_v)):
        part = dot(spread, w[...]).reshape(n_ep, rows, local)
        q_send[:, :, j * local : (j + 1) * local] = part.astype(BF)
    wait_q = exchange(ep_copy, 1, ep_peers, me, lambda p: q_send.at[p], q_recv)
    q_recv[me] = q_send[me]
    loads[state_i].wait()
    wait_q()
    wait_c = exchange(ep_copy, 2, ep_peers, me, lambda p: c_send.at[p], c_recv)
    c_recv[me] = c_send[me]

    summed = q_recv[0].astype(F32)
    for p in range(1, n_ep):
        summed = summed + q_recv[p].astype(F32)
    summed = summed.astype(BF).astype(F32)

    def head_of(which, h):
        return summed[:, which * local + h * 128 : which * local + (h + 1) * 128]

    def unit(values):
        return values * lax.rsqrt(jnp.sum(values * values, axis=-1, keepdims=True) + EPS)

    units = []
    for h in range(heads):
        q_unit = unit(head_of(0, h)) * 128 ** (-0.5)
        k_unit = unit(head_of(1, h))
        units.append((q_unit, k_unit))
        kq[:, h, :] = k_unit
        kq[:, heads + h, :] = q_unit

    def one_row(b, _):
        columns = kq[b].T
        for h in range(heads):
            block = state[b, h]
            recall[h, pl.ds(b, 1), :] = jnp.sum(columns[:, h : h + 1] * block, axis=0, keepdims=True)
            recall[heads + h, pl.ds(b, 1), :] = jnp.sum(
                columns[:, heads + h : heads + h + 1] * block, axis=0, keepdims=True
            )
        return 0

    lax.fori_loop(0, rows, one_row, 0)
    for h in range(heads):
        q_unit, k_unit = units[h]
        decay, beta = decays[h], betas[h]
        corr = beta * (head_of(2, h) - decay * recall[h])
        read = decay * recall[heads + h] + jnp.sum(q_unit * k_unit, axis=-1, keepdims=True) * corr
        read = read * lax.rsqrt(jnp.mean(read * read, axis=-1, keepdims=True) + EPS) * head_gain[...]
        head_out[:, h * 128 : (h + 1) * 128] = read.astype(BF)
        key_out[:, h, :] = k_unit
        corr_out[:, h, :] = corr
        decay_out[:, h, :] = jnp.broadcast_to(decay, (rows, 128))

    loads[o_i].wait()
    ho = head_out[...]
    for c in range(n_tp):
        a_send[c] = dot(ho, w_o[:, c * chunk : (c + 1) * chunk]).astype(BF)
    wait_a = exchange(tp_copy, 0, tp_peers, my, lambda p: a_send.at[p], a_recv)
    a_recv[my] = a_send[my]
    own = pl.ds(pl.multiple_of(my * chunk, 128), chunk)
    middle = tokens[:, own].astype(F32)
    wait_a()
    for p in range(n_tp):
        middle = middle + a_recv[p].astype(F32)
    middle_ref[...] = middle
    s_recv[my] = jnp.broadcast_to(jnp.sum(middle * middle, axis=-1, keepdims=True), (rows, 128))
    wait_s = exchange(tp_copy, 1, tp_peers, my, lambda p: s_recv.at[my], s_recv)
    wait_c()
    coef = c_recv[...].reshape(batch, 128)[:, :1]
    named = coef > 0.0
    tri = (
        lax.broadcasted_iota(jnp.int32, (batch, batch), 0)
        >= lax.broadcasted_iota(jnp.int32, (batch, batch), 1)
    ).astype(F32).astype(BF)
    flags = jnp.broadcast_to(jnp.where(named, 1.0, 0.0), (batch, 128)).astype(BF)
    rank = dot(tri, flags)[:, :1] - 1.0
    slot = lax.broadcasted_iota(jnp.int32, (batch, slots), 1).astype(F32)
    place = jnp.where((rank == slot) & named, 1.0, 0.0).astype(BF)
    wait_s()
    total = s_recv[0]
    for p in range(1, n_tp):
        total = total + s_recv[p]
    scale = lax.rsqrt(total[:, :1] / width + EPS)
    x_all[me] = (middle * scale * ffn_gain[:, own]).astype(BF)
    wait_x = exchange(ep_copy, 3, ep_peers, me, lambda p: x_all.at[me], x_all)
    for i in (dg_i, du_i, eg_i, eu_i, ed_i, dd_i):
        loads[i].wait()
    wait_x()

    xs = x_all[...].astype(F32).reshape(batch, chunk).astype(BF)
    g_all[my] = lax.dot_general(
        place, xs, (((0,), (0,)), ((), ())), preferred_element_type=F32
    ).astype(BF)
    wait_g = exchange(tp_copy, 2, tp_peers, my, lambda p: g_all.at[my], g_all)
    hidden = w_dg.shape[1]
    part_rows = batch // n_tp
    for j, w in enumerate((w_dg, w_du)):
        part = dot(xs, w[...]).reshape(n_tp, part_rows, hidden)
        d_send[:, :, j * hidden : (j + 1) * hidden] = part.astype(BF)
    wait_d = exchange(tp_copy, 3, tp_peers, my, lambda p: d_send.at[p], d_recv)
    d_recv[my] = d_send[my]

    wait_g()
    gate = jnp.zeros((slots, w_eg.shape[2]), F32)
    up = jnp.zeros((slots, w_eg.shape[2]), F32)
    for c in range(n_tp):
        gate = gate + dot(g_all[c], w_eg[0, c * chunk : (c + 1) * chunk, :])
        up = up + dot(g_all[c], w_eu[0, c * chunk : (c + 1) * chunk, :])
    expert_hidden = (silu(gate) * up).astype(BF)
    for c in range(n_tp):
        e_send[c] = dot(expert_hidden, w_ed[0, :, c * chunk : (c + 1) * chunk]).astype(BF)
    wait_e = exchange(tp_copy, 4, tp_peers, my, lambda p: e_send.at[p], e_recv)
    e_recv[my] = e_send[my]

    wait_d()
    pre = d_recv[0].astype(F32)
    for p in range(1, n_tp):
        pre = pre + d_recv[p].astype(F32)
    h_all[my] = (silu(pre[:, :hidden]) * pre[:, hidden:]).astype(BF)
    wait_h = exchange(tp_copy, 5, tp_peers, my, lambda p: h_all.at[my], h_all)
    wait_h()
    dense_hidden = h_all[...].astype(F32).reshape(batch, hidden).astype(BF)
    dense = dot(dense_hidden, w_dd[...]) * (1.0 / (1.0 + jnp.exp(-mix[...])))
    wait_e()
    result = e_recv[0].astype(F32)
    for p in range(1, n_tp):
        result = result + e_recv[p].astype(F32)
    combined = dense + coef * dot(place, result.astype(BF))
    f_send[...] = combined.reshape(n_ep, rows, chunk).astype(BF)
    wait_f = exchange(ep_copy, 4, ep_peers, me, lambda p: f_send.at[p], f_recv)
    final = middle_ref[...] + f_send[me].astype(F32)
    f_recv[me] = jnp.zeros((rows, chunk), BF)
    wait_f()
    for p in range(n_ep):
        final = final + f_recv[p].astype(F32)
    out[...] = final.astype(BF)


def per_device(
    tokens, delta_state, attn_gain, query_weight, key_weight, value_weight, decay_weight,
    beta_weight, decay_rate, head_gain, output_weight, ffn_gain, expert_ids, group_prob,
    expert_logit, expert_gate, expert_up, expert_down, dense_gate, dense_up, dense_down, dense_mix,
):
    n_ep = lax.axis_size("ep")
    n_tp = lax.axis_size("tp")
    rows, width = tokens.shape
    heads = delta_state.shape[1]
    local = heads * 128
    topk = expert_ids.shape[1]
    slots = max(2, 2 * rows * topk // n_ep) * n_ep
    chunk = width // n_tp
    depth = width // n_ep
    batch = n_ep * rows
    hidden = dense_gate.shape[1]
    small = (
        tokens, attn_gain[None, :], decay_rate[None, :], head_gain[None, :], ffn_gain[None, :],
        expert_ids, group_prob[:, None], expert_logit, dense_mix[None, :],
    )
    weights = (
        delta_state, decay_weight, beta_weight, query_weight, key_weight, value_weight,
        output_weight, dense_gate, dense_up, expert_gate, expert_up, expert_down, dense_down,
    )
    dims = (n_ep, n_tp, rows, width, heads, slots, topk, len(small) + len(weights), len(weights))
    vmem = pl.BlockSpec(memory_space=pltpu.VMEM)
    kq_rows = -(-2 * heads // 8) * 8
    scratch = [pltpu.VMEM(w.shape, w.dtype) for w in weights]
    scratch += [
        pltpu.VMEM(shape, dtype)
        for shape, dtype in (
            ((n_ep, rows, depth), BF), ((n_ep, rows, depth), BF),
            ((n_ep, rows, 3 * local), BF), ((n_ep, rows, 3 * local), BF),
            ((n_ep, rows, 128), F32), ((n_ep, rows, 128), F32),
            ((rows, kq_rows, 128), F32), ((2 * heads, rows, 128), F32), ((rows, local), BF),
            ((n_tp, rows, chunk), BF), ((n_tp, rows, chunk), BF), ((n_tp, rows, 128), F32),
            ((rows, chunk), F32), ((n_ep, rows, chunk), BF), ((n_tp, slots, chunk), BF),
            ((n_tp, batch // n_tp, 2 * hidden), BF), ((n_tp, batch // n_tp, 2 * hidden), BF),
            ((n_tp, batch // n_tp, hidden), BF),
            ((n_tp, slots, chunk), BF), ((n_tp, slots, chunk), BF),
            ((n_ep, rows, chunk), BF), ((n_ep, rows, chunk), BF),
        )
    ]
    scratch += [
        pltpu.SemaphoreType.DMA((len(weights),)),
        pltpu.SemaphoreType.DMA((5, n_ep)), pltpu.SemaphoreType.DMA((5, n_ep)),
        pltpu.SemaphoreType.DMA((6, n_tp)), pltpu.SemaphoreType.DMA((6, n_tp)),
    ]
    per_head = jax.ShapeDtypeStruct((rows, heads, 128), F32)
    mixed_out, key, corr, decay = pl.pallas_call(
        functools.partial(kernel, dims),
        out_shape=(jax.ShapeDtypeStruct((rows, chunk), BF), per_head, per_head, per_head),
        in_specs=[vmem] * len(small) + [pl.BlockSpec(memory_space=pl.ANY)] * len(weights),
        out_specs=(vmem,) * 4,
        scratch_shapes=scratch,
        compiler_params=pltpu.CompilerParams(
            collective_id=0, has_side_effects=True, vmem_limit_bytes=62 * 1024 * 1024
        ),
    )(*small, *weights)
    new_state = decay[:, :, None, :] * delta_state + key[..., :, None] * corr[..., None, :]
    return mixed_out, new_state


def solution(mesh):
    return jax.shard_map(
        per_device,
        mesh=mesh,
        in_specs=(
            P("ep", None), P("ep", "tp", None, None), P(), P("ep", "tp"), P("ep", "tp"),
            P("ep", "tp"), P(), P(), P("tp"), P(), P("tp", None), P(), P("ep", None), P("ep"),
            P("ep", None), P("ep", None, "tp"), P("ep", None, "tp"), P("ep", "tp", None),
            P("tp", "ep"), P("tp", "ep"), P("ep", "tp"), P("tp"),
        ),
        out_specs=(P("ep", "tp"), P("ep", "tp", None, None)),
        check_vma=False,
    )
```

```python
import functools
import math

import jax
import jax.numpy as jnp
from jax import lax
from jax.experimental import pallas as pl
from jax.experimental.pallas import tpu as pltpu
from jax.sharding import PartitionSpec as P

EPS = 1e-06
BF = jnp.bfloat16
F32 = jnp.float32
MESH = pl.DeviceIdType.MESH


def dot(left, right):
    return jnp.dot(left, right, preferred_element_type=F32)


def dot_t(left, right):
    return lax.dot_general(left, right, (((1,), (1,)), ((), ())), preferred_element_type=F32)


def silu(values):
    return values / (1.0 + jnp.exp(-values))


class BlockOf:
    def __init__(self, ref, block):
        self.ref, self.block = ref, block

    @property
    def at(self):
        return self

    def __getitem__(self, index):
        return self.ref.at[index, self.block]


def kernel(dims, *refs):
    n_ep, n_tp, rows, width, heads, members, cap, n_in, n_weights = dims
    inputs, refs = refs[:n_in], refs[n_in:]
    (tokens, attn_gain, decay_rate, head_gain, ffn_gain, ids, group_prob, logit, mix) = inputs[:9]
    hbm = inputs[9:]
    out, key_out, corr_out, decay_out = refs[:4]
    held = refs[4 : 4 + n_weights]
    refs = refs[4 + n_weights :]
    state, w_decay, w_beta, w_q, w_k, w_v, w_o, w_dg, w_du, w_eg, w_eu, w_ed, w_dd = held
    (
        n_send, n_recv, q_send, q_recv, c_send, c_recv, kq, recall, head_out,
        a_send, a_recv, s_recv, middle_ref, x_all, g_all, d_send, d_recv, h_all,
        e_send, e_recv, f_send, f_recv, place_ref, dense_ref, load_sem, ep_send, ep_recv, tp_send, tp_recv,
    ) = refs
    me = lax.axis_index("ep")
    my = lax.axis_index("tp")
    chunk = width // n_tp
    depth = width // n_ep
    batch = n_ep * rows
    local = heads * 128
    groups = n_ep // members
    group_slots = members * cap
    group_tokens = members * rows
    slots = groups * group_slots
    my_group = lax.div(me, members)
    my_member = lax.rem(me, members)

    def members_of(offset):
        first = lax.rem(my_group + offset + groups, groups) * members
        start = 1 if offset == 0 else 0
        return [first + lax.rem(my_member + m, members) for m in range(start, members)]

    loads = [
        pltpu.make_async_copy(src, dst, load_sem.at[i])
        for i, (src, dst) in enumerate(zip(hbm, held))
    ]
    state_i, decay_i, beta_i, q_i, k_i, v_i, o_i, dg_i, du_i, eg_i, eu_i, ed_i, dd_i = range(13)
    order = (decay_i, beta_i, q_i, k_i, v_i, state_i, o_i, dg_i, du_i, eg_i, eu_i, ed_i, dd_i)

    ep_peers = [p for offset in range(groups) for p in members_of(offset)]
    tp_peers = [lax.rem(my + d, n_tp) for d in range(1, n_tp)]
    barrier = pltpu.get_barrier_semaphore()
    for p in ep_peers:
        pl.semaphore_signal(barrier, inc=1, device_id=(p, my), device_id_type=MESH)
    for p in tp_peers:
        pl.semaphore_signal(barrier, inc=1, device_id=(me, p), device_id_type=MESH)
    for i in order:
        loads[i].start()

    def ep_copy(phase, src, dst, peer, source):
        return pltpu.make_async_remote_copy(
            src_ref=src, dst_ref=dst,
            send_sem=ep_send.at[phase, peer], recv_sem=ep_recv.at[phase, source],
            device_id=(peer, my), device_id_type=MESH,
        )

    def tp_copy(phase, src, dst, peer, source):
        return pltpu.make_async_remote_copy(
            src_ref=src, dst_ref=dst,
            send_sem=tp_send.at[phase, peer], recv_sem=tp_recv.at[phase, source],
            device_id=(me, peer), device_id_type=MESH,
        )

    def exchange(copy, phase, peers, mine, src_of, dst):
        for p in peers:
            copy(phase, src_of(p), dst.at[mine], p, mine).start()

        def arrived():
            for p in peers:
                done = copy(phase, src_of(p), dst.at[p], p, p)
                done.wait_recv()
                done.wait_send()

        return arrived

    x = tokens[...].astype(F32)
    mean_sq = jnp.mean(x * x, axis=-1, keepdims=True)
    normed = (x * lax.rsqrt(mean_sq + EPS) * attn_gain[...]).astype(BF)
    for p in range(n_ep):
        n_send[p] = normed[:, p * depth : (p + 1) * depth]
    pl.semaphore_wait(barrier, n_ep + n_tp - 2)
    wait_n = exchange(ep_copy, 0, ep_peers, me, lambda p: n_send.at[p], n_recv)
    n_recv[me] = n_send[me]

    logit_exp = jnp.exp(logit[...])
    route = group_prob[...] * logit_exp / jnp.sum(logit_exp, axis=0, keepdims=True)
    names = ids[...]
    eye = lax.broadcasted_iota(jnp.int32, (rows, rows), 0) == lax.broadcasted_iota(
        jnp.int32, (rows, rows), 1
    )
    for p in range(n_ep):
        flat = jnp.sum(jnp.where(names == p, route, 0.0), axis=0, keepdims=True)
        coef = jnp.sum(jnp.where(eye, flat, 0.0), axis=1, keepdims=True)
        c_send[p] = jnp.broadcast_to(coef, (rows, 128))
    loads[decay_i].wait()
    loads[beta_i].wait()
    decay_pre = dot_t(normed, w_decay[...])
    beta_pre = dot_t(normed, w_beta[...])
    lane = lax.broadcasted_iota(jnp.int32, decay_pre.shape, 1)
    decays, betas = [], []
    for h in range(heads):
        mine = lane == my * heads + h
        d = jnp.sum(jnp.where(mine, decay_pre, 0.0), axis=1, keepdims=True)
        b = jnp.sum(jnp.where(mine, beta_pre, 0.0), axis=1, keepdims=True)
        soft = jnp.maximum(d, 0.0) + jnp.log1p(jnp.exp(-jnp.abs(d)))
        decays.append(jnp.exp(-decay_rate[:, h : h + 1] * soft))
        betas.append(1.0 / (1.0 + jnp.exp(-b)))
    for i in (q_i, k_i, v_i):
        loads[i].wait()

    wait_n()
    spread = n_recv[...].astype(F32).reshape(batch, depth).astype(BF)
    wait_heads = []
    for j, w in enumerate((w_k, w_q, w_v)):
        part = dot(spread, w[...]).reshape(n_ep, rows, local)
        q_send[j] = part.astype(BF)
        wait_heads.append(
            exchange(ep_copy, 1 + j, ep_peers, me, lambda p, j=j: q_send.at[j, p], q_recv.at[j])
        )
        q_recv[j, me] = q_send[j, me]

    def summed(j):
        wait_heads[j]()
        total = q_recv[j, 0].astype(F32)
        for p in range(1, n_ep):
            total = total + q_recv[j, p].astype(F32)
        return total.astype(BF).astype(F32)

    k_rows = summed(0)
    q_rows = summed(1)
    loads[state_i].wait()

    def head_of(values, h):
        return values[:, h * 128 : (h + 1) * 128]

    def unit(values):
        return values * lax.rsqrt(jnp.sum(values * values, axis=-1, keepdims=True) + EPS)

    units = []
    for h in range(heads):
        q_unit = unit(head_of(q_rows, h)) * 128 ** (-0.5)
        k_unit = unit(head_of(k_rows, h))
        units.append((q_unit, k_unit))
        kq[:, h, :] = k_unit
        kq[:, heads + h, :] = q_unit

    def one_row(b, _):
        columns = kq[b].T
        for h in range(heads):
            block = state[b, h]
            recall[h, pl.ds(b, 1), :] = jnp.sum(columns[:, h : h + 1] * block, axis=0, keepdims=True)
            recall[heads + h, pl.ds(b, 1), :] = jnp.sum(
                columns[:, heads + h : heads + h + 1] * block, axis=0, keepdims=True
            )
        return 0

    lax.fori_loop(0, rows, one_row, 0)
    v_rows = summed(2)
    wait_c = exchange(ep_copy, 4, ep_peers, me, lambda p: c_send.at[p], c_recv)
    c_recv[me] = c_send[me]
    for h in range(heads):
        q_unit, k_unit = units[h]
        decay, beta = decays[h], betas[h]
        corr = beta * (head_of(v_rows, h) - decay * recall[h])
        read = decay * recall[heads + h] + jnp.sum(q_unit * k_unit, axis=-1, keepdims=True) * corr
        read = read * lax.rsqrt(jnp.mean(read * read, axis=-1, keepdims=True) + EPS) * head_gain[...]
        head_out[:, h * 128 : (h + 1) * 128] = read.astype(BF)
        key_out[:, h, :] = k_unit
        corr_out[:, h, :] = corr
        decay_out[:, h, :] = jnp.broadcast_to(decay, (rows, 128))

    loads[o_i].wait()
    ho = head_out[...]
    for c in range(n_tp):
        a_send[c] = dot(ho, w_o[:, c * chunk : (c + 1) * chunk]).astype(BF)
    wait_a = exchange(tp_copy, 0, tp_peers, my, lambda p: a_send.at[p], a_recv)
    a_recv[my] = a_send[my]
    own = pl.ds(pl.multiple_of(my * chunk, 128), chunk)
    middle = tokens[:, own].astype(F32)
    wait_a()
    for p in range(n_tp):
        middle = middle + a_recv[p].astype(F32)
    middle_ref[...] = middle
    s_recv[my] = jnp.broadcast_to(jnp.sum(middle * middle, axis=-1, keepdims=True), (rows, 128))
    wait_s = exchange(tp_copy, 1, tp_peers, my, lambda p: s_recv.at[my], s_recv)
    wait_c()
    tri = (
        lax.broadcasted_iota(jnp.int32, (group_tokens, group_tokens), 0)
        >= lax.broadcasted_iota(jnp.int32, (group_tokens, group_tokens), 1)
    ).astype(F32).astype(BF)
    slot = lax.broadcasted_iota(jnp.int32, (group_tokens, group_slots), 1).astype(F32)
    for g in range(groups):
        coef = c_recv[g * members : (g + 1) * members].reshape(group_tokens, 128)[:, :1]
        named = coef > 0.0
        flags = jnp.broadcast_to(jnp.where(named, 1.0, 0.0), (group_tokens, 128)).astype(BF)
        rank = dot(tri, flags)[:, :1] - 1.0
        place_ref[g] = jnp.where((rank == slot) & named, 1.0, 0.0).astype(BF)
    wait_s()
    total = s_recv[0]
    for p in range(1, n_tp):
        total = total + s_recv[p]
    scale = lax.rsqrt(total[:, :1] / width + EPS)
    x_all[me] = (middle * scale * ffn_gain[:, own]).astype(BF)
    for p in ep_peers:
        ep_copy(5, x_all.at[me], x_all.at[me], p, me).start()
    wait_g = []
    for offset in range(groups):
        g = lax.rem(my_group - offset + groups, groups)
        for p in members_of(-offset):
            ep_copy(5, x_all.at[me], x_all.at[p], p, p).wait_recv()
        block = x_all[pl.ds(g * members, members)].astype(F32)
        g_all[my, g] = lax.dot_general(
            place_ref[g], block.reshape(group_tokens, chunk).astype(BF),
            (((0,), (0,)), ((), ())), preferred_element_type=F32,
        ).astype(BF)
        wait_g.append(
            exchange(
                tp_copy, 4 + offset, tp_peers, my, lambda p, g=g: g_all.at[my, g],
                BlockOf(g_all, g),
            )
        )
    for p in ep_peers:
        ep_copy(5, x_all.at[me], x_all.at[me], p, me).wait_send()
    for i in (dg_i, du_i, eg_i, eu_i, ed_i, dd_i):
        loads[i].wait()
    xs = x_all[...].astype(F32).reshape(batch, chunk).astype(BF)
    hidden = w_dg.shape[1]
    part_rows = batch // n_tp
    for j, w in enumerate((w_dg, w_du)):
        part = dot(xs, w[...]).reshape(n_tp, part_rows, hidden)
        d_send[:, :, j * hidden : (j + 1) * hidden] = part.astype(BF)
    wait_d = exchange(tp_copy, 2, tp_peers, my, lambda p: d_send.at[p], d_recv)
    d_recv[my] = d_send[my]

    for wait in wait_g:
        wait()
    gate = jnp.zeros((slots, w_eg.shape[2]), F32)
    up = jnp.zeros((slots, w_eg.shape[2]), F32)
    for c in range(n_tp):
        routed = g_all[c].astype(F32).reshape(slots, chunk).astype(BF)
        gate = gate + dot(routed, w_eg[0, c * chunk : (c + 1) * chunk, :])
        up = up + dot(routed, w_eu[0, c * chunk : (c + 1) * chunk, :])
    expert_hidden = (silu(gate) * up).astype(BF)
    for c in range(n_tp):
        part = dot(expert_hidden, w_ed[0, :, c * chunk : (c + 1) * chunk])
        e_send[c] = part.reshape(groups, group_slots, chunk).astype(BF)
    e_recv[my] = e_send[my]
    returns = list(range(1, groups)) + [0]
    group_at = [lax.rem(my_group + offset, groups) for offset in range(groups)]

    def send_e(offset):
        g = group_at[offset]
        return exchange(
            tp_copy, 4 + groups + offset, tp_peers, my, lambda p: e_send.at[p, g],
            BlockOf(e_recv, g),
        )

    wait_e = {returns[0]: send_e(returns[0])}
    wait_d()
    pre = d_recv[0].astype(F32)
    for p in range(1, n_tp):
        pre = pre + d_recv[p].astype(F32)
    h_all[my] = (silu(pre[:, :hidden]) * pre[:, hidden:]).astype(BF)
    wait_h = exchange(tp_copy, 3, tp_peers, my, lambda p: h_all.at[my], h_all)
    for offset in returns[1:]:
        wait_e[offset] = send_e(offset)
    wait_h()
    dense_hidden = h_all[...].astype(F32).reshape(batch, hidden).astype(BF)
    dense = dot(dense_hidden, w_dd[...]) * (1.0 / (1.0 + jnp.exp(-mix[...])))
    dense_ref[...] = dense.reshape(n_ep, rows, chunk)
    for offset in returns:
        g = group_at[offset]
        here = pl.ds(g * members, members)
        wait_e[offset]()
        result = e_recv[0, g].astype(F32)
        for p in range(1, n_tp):
            result = result + e_recv[p, g].astype(F32)
        coef = c_recv[here].reshape(group_tokens, 128)[:, :1]
        mixed = coef * dot(place_ref[g], result.astype(BF))
        combined = dense_ref[here] + mixed.reshape(members, rows, chunk)
        f_send[here] = combined.astype(BF)
        for p in members_of(offset):
            ep_copy(6, f_send.at[p], f_recv.at[me], p, me).start()
    final = middle_ref[...] + f_send[me].astype(F32)
    f_recv[me] = jnp.zeros((rows, chunk), BF)
    for p in ep_peers:
        done = ep_copy(6, f_send.at[p], f_recv.at[p], p, p)
        done.wait_recv()
        done.wait_send()
    for p in range(n_ep):
        final = final + f_recv[p].astype(F32)
    out[...] = final.astype(BF)


def per_device(
    tokens, delta_state, attn_gain, query_weight, key_weight, value_weight, decay_weight,
    beta_weight, decay_rate, head_gain, output_weight, ffn_gain, expert_ids, group_prob,
    expert_logit, expert_gate, expert_up, expert_down, dense_gate, dense_up, dense_down, dense_mix,
):
    n_ep = lax.axis_size("ep")
    n_tp = lax.axis_size("tp")
    rows, width = tokens.shape
    heads = delta_state.shape[1]
    local = heads * 128
    topk = expert_ids.shape[1]
    cap = max(2, 2 * rows * topk // n_ep)
    members = 8 // math.gcd(cap, 8)
    if n_ep % members:
        members = n_ep
    groups = n_ep // members
    group_slots = members * cap
    chunk = width // n_tp
    depth = width // n_ep
    batch = n_ep * rows
    hidden = dense_gate.shape[1]
    small = (
        tokens, attn_gain[None, :], decay_rate[None, :], head_gain[None, :], ffn_gain[None, :],
        expert_ids.T, group_prob[None, :], expert_logit.T, dense_mix[None, :],
    )
    weights = (
        delta_state, decay_weight.T, beta_weight.T, query_weight, key_weight, value_weight,
        output_weight, dense_gate, dense_up, expert_gate, expert_up, expert_down, dense_down,
    )
    dims = (n_ep, n_tp, rows, width, heads, members, cap, len(small) + len(weights), len(weights))
    vmem = pl.BlockSpec(memory_space=pltpu.VMEM)
    kq_rows = -(-2 * heads // 8) * 8
    scratch = [pltpu.VMEM(w.shape, w.dtype) for w in weights]
    scratch += [
        pltpu.VMEM(shape, dtype)
        for shape, dtype in (
            ((n_ep, rows, depth), BF), ((n_ep, rows, depth), BF),
            ((3, n_ep, rows, local), BF), ((3, n_ep, rows, local), BF),
            ((n_ep, rows, 128), F32), ((n_ep, rows, 128), F32),
            ((rows, kq_rows, 128), F32), ((2 * heads, rows, 128), F32), ((rows, local), BF),
            ((n_tp, rows, chunk), BF), ((n_tp, rows, chunk), BF), ((n_tp, rows, 128), F32),
            ((rows, chunk), F32), ((n_ep, rows, chunk), BF), ((n_tp, groups, group_slots, chunk), BF),
            ((n_tp, batch // n_tp, 2 * hidden), BF), ((n_tp, batch // n_tp, 2 * hidden), BF),
            ((n_tp, batch // n_tp, hidden), BF),
            ((n_tp, groups, group_slots, chunk), BF), ((n_tp, groups, group_slots, chunk), BF),
            ((n_ep, rows, chunk), BF), ((n_ep, rows, chunk), BF),
            ((groups, members * rows, group_slots), BF), ((n_ep, rows, chunk), F32),
        )
    ]
    scratch += [
        pltpu.SemaphoreType.DMA((len(weights),)),
        pltpu.SemaphoreType.DMA((7, n_ep)), pltpu.SemaphoreType.DMA((7, n_ep)),
        pltpu.SemaphoreType.DMA((4 + 2 * groups, n_tp)), pltpu.SemaphoreType.DMA((4 + 2 * groups, n_tp)),
    ]
    per_head = jax.ShapeDtypeStruct((rows, heads, 128), F32)
    mixed_out, key, corr, decay = pl.pallas_call(
        functools.partial(kernel, dims),
        out_shape=(jax.ShapeDtypeStruct((rows, chunk), BF), per_head, per_head, per_head),
        in_specs=[vmem] * len(small) + [pl.BlockSpec(memory_space=pl.ANY)] * len(weights),
        out_specs=(vmem,) * 4,
        scratch_shapes=scratch,
        compiler_params=pltpu.CompilerParams(
            collective_id=0, has_side_effects=True, vmem_limit_bytes=62 * 1024 * 1024
        ),
    )(*small, *weights)
    new_state = decay[:, :, None, :] * delta_state + key[..., :, None] * corr[..., None, :]
    return mixed_out, new_state


def solution(mesh):
    return jax.shard_map(
        per_device,
        mesh=mesh,
        in_specs=(
            P("ep", None), P("ep", "tp", None, None), P(), P("ep", "tp"), P("ep", "tp"),
            P("ep", "tp"), P(), P(), P("tp"), P(), P("tp", None), P(), P("ep", None), P("ep"),
            P("ep", None), P("ep", None, "tp"), P("ep", None, "tp"), P("ep", "tp", None),
            P("tp", "ep"), P("tp", "ep"), P("ep", "tp"), P("tp"),
        ),
        out_specs=(P("ep", "tp"), P("ep", "tp", None, None)),
        check_vma=False,
    )
```
